32 devices in a mesh: grp: 2 (over y), ep: 4 (over z), tp: 4 (over x, core).
Axes of the slice: x: 2, y: 2, z: 4, core: 2. Of those that a mesh axis runs over, the one named last changes fastest.
Arguments:
- tokens: bfloat16 [2048, 2048], P(('grp', 'ep', 'tp')), parts along dimension 0, may hold values from -6 to 6
- gain_in: float32 [2048], replicated, may hold values from 0.1 to 1.9
- routes: int32 [2048, 2], P(('grp', 'ep')), parts along dimension 0, may hold values from 0 to 3, all different within a row; in each aligned block of 64 rows (0 to 63, 64 to 127, ...) at most 48 rows name the same one
- gates: float32 [2048, 2], P(('grp', 'ep')), parts along dimension 0, may hold values from 0.05 to 1
- w_gate: bfloat16 [4, 2048, 3072], P('ep', None, 'tp'), may hold values from -0.125 to 0.125
- w_up: bfloat16 [4, 2048, 3072], P('ep', None, 'tp'), may hold values from -0.125 to 0.125
- w_down: bfloat16 [4, 3072, 2048], P('ep', 'tp'), may hold values from -0.109375 to 0.109375
- gain_out: float32 [2048], P('tp'), may hold values from 0.3 to 3
Outputs:
- mixed: bfloat16 [2048, 2048], P(('grp', 'ep'), 'tp'), parts along dimension 0
The draws below stay inside these ranges and needn't reach their ends.
There are 2 independent parts, one for each index of `grp`. The reference program is written for one: setup_inputs(seed, part) draws one part's arguments, and reference() takes and returns one part's arrays. A program takes and returns all parts, laid end to end along the dimension named above; an argument that names none is the same for every part. Nothing has to cross between parts.
Inputs may be any that keep to these rules, and one draw needn't show every extreme that they name: `routes`: each row names 2 different experts; every expert is named by some row. Among the rows of one device (aligned blocks of 64 rows) no expert is named more than 48 times, and in every draw some expert is named exactly 48 times in some such block.
All inputs are finite; a program needn't handle non-finite values.
Results may differ from the reference program's by a relative error of at most 0.012.
Values may be sent and summed in bfloat16 or wider, within the bound.
A program may use at most 64 MiB of HBM per device.

```python
import math
import jax
import jax.numpy as jnp
import numpy as np
from jax import lax

D = 2048
FF = 3072
TOPK = 2
TOK_DEV = 64
EXPERTS = 4
CAP = 48
FF_DEV = 768
TOKENS = 1024
N_EP = 4
N_TP = 4


def level_of(own_key, extent, split, smallest, top_value):
    level = 1.0
    for dim, blocks in split:
        heights = jax.random.uniform(jax.random.fold_in(jax.random.fold_in(own_key, 6), dim), (blocks,), jnp.float32, smallest / len(split), top_value / len(split))
        level = level * jnp.repeat(jnp.exp(heights), extent[dim] // blocks).reshape((-1,) + (1,) * (len(extent) - 1 - dim))
    return level


def deal_out(rng, own, number, rows, amount, top, reach, lean):
    sequence = jax.random.permutation(rng, amount)
    crowded, common = load_shares(amount, rows * top, reach, lean, True), load_shares(amount, rows * top, reach, lean, False)
    places = jnp.arange(amount)

    def named(tallies, turn):
        used = int((tallies > 0).sum())
        fixed = max(1, used // 4)
        passed = fixed + (places - fixed + turn * (used - fixed)) % max(1, amount - fixed)
        return jnp.zeros((amount,), jnp.int32).at[sequence[jnp.where(places < fixed, places, passed)]].set(jnp.asarray(tallies, jnp.int32))

    tallies = jnp.where(number % 4 == 0, named(crowded, number // 4), named(common, number - number // 4 - 1))
    mixed = jax.random.permutation(jax.random.fold_in(own, 3), amount)
    donor, taker = mixed[0:amount // 2 * 2:2], mixed[1:amount // 2 * 2:2]
    slack = jnp.minimum(tallies[donor] - 1, reach - tallies[taker]) // 2
    slack = jnp.where((donor == sequence[0]) | (taker == sequence[0]) | (tallies[taker] == 0), 0, jnp.maximum(slack, 0))
    passed = jax.random.randint(jax.random.fold_in(own, 4), (amount // 2,), 0, 1 << 20) % (slack + 1)
    tallies = tallies.at[donor].add(-passed).at[taker].add(passed)
    members = jnp.searchsorted(jnp.cumsum(tallies), jnp.arange(rows * top), side="right").astype(jnp.int32)
    listing = members.reshape(top, rows).T
    listing = listing[jax.random.permutation(jax.random.fold_in(own, 1), rows)]
    turn = jax.random.randint(jax.random.fold_in(own, 2), (rows, 1), 0, top)
    return jnp.take_along_axis(listing, (jnp.arange(top)[None, :] + turn) % top, axis=1)


def load_shares(number_of, total, reach, slope, full):
    portions = [(1 << 20) // math.isqrt(standing ** slope) + 1 for standing in range(1, number_of + 1)]
    largest = reach if full else min(reach, max(-(-total // number_of), total * portions[0] // sum(portions)))
    least = 1 if total - largest >= number_of - 1 else 0
    holding, spare = [largest] + [least] * (number_of - 1), total - largest - least * (number_of - 1)
    while spare > 0:
        movable = [i for i in range(1, number_of) if holding[i] < largest] or [i for i in range(1, number_of) if holding[i] < reach]
        pool, remaining = sum([portions[i] for i in movable]), spare
        for i in movable:
            extra = min(reach - holding[i], max(1, remaining * portions[i] // pool), spare)
            holding[i] = holding[i] + extra
            spare = spare - extra
    return np.array(holding)


def bell_draw(own_key, shape, scale, reach, pieces=(), held_as=jnp.bfloat16):
    values = jax.random.normal(own_key, shape, jnp.float32) * scale
    if len(pieces) > 0:
        values = level_of(own_key, shape, pieces, -0.22, 0.18) * values
    return jnp.clip(values, min=-reach, max=reach).astype(held_as)


def setup_inputs(seed: int = 0, part: int = 0) -> dict:
    streams_of = jax.random.split(jax.random.key(seed), 9)
    part_keys = jax.random.split(jax.random.fold_in(streams_of[8], part), 9)
    tokens = bell_draw(part_keys[0], (TOKENS, D), 1.0, 6.0, ((0, 16),))
    gain_in = jnp.clip(1.0 + 0.18 * jax.random.normal(streams_of[1], (D,), jnp.float32), 0.1, 1.9)
    routes_keys = jax.random.split(jax.random.fold_in(part_keys[2], 1), TOKENS // TOK_DEV)
    routes_turns = jax.random.permutation(jax.random.fold_in(part_keys[2], 3), TOKENS // TOK_DEV)
    routes = jax.vmap(lambda own, number: deal_out(jax.random.fold_in(part_keys[2], 2), own, number, TOK_DEV, EXPERTS, TOPK, CAP, 2))(routes_keys, routes_turns).reshape((TOKENS, TOPK))
    gates = jnp.clip(0.05 + 0.95 * jax.random.uniform(part_keys[3], (TOKENS, TOPK), jnp.float32) ** level_of(part_keys[3], (TOKENS, TOPK), ((0, 4),), -0.2, 0.2), 0.05, 1.0)
    w_gate = bell_draw(streams_of[4], (EXPERTS, D, FF), D ** -0.5, 0.125, ((0, 4), (2, 4)))
    w_up = bell_draw(streams_of[5], (EXPERTS, D, FF), D ** -0.5, 0.125, ((0, 4), (2, 4)))
    w_down = bell_draw(streams_of[6], (EXPERTS, FF, D), FF ** -0.5, 0.109375, ((0, 4), (1, 4)))
    gain_out = jnp.clip(jnp.exp(math.log(3.0) - 2.3025851 * jax.random.uniform(streams_of[7], (D,), jnp.float32) ** level_of(streams_of[7], (D,), ((0, 4),), -0.2, 0.2)), 0.3, 3.0)
    return {"tokens": tokens, "gain_in": gain_in, "routes": routes, "gates": gates, "w_gate": w_gate, "w_up": w_up, "w_down": w_down, "gain_out": gain_out}


EPS = 1e-06

def reference(tokens, gain_in, routes, gates, w_gate, w_up, w_down, gain_out):
    values = tokens.astype(jnp.float32)
    normed = (values * lax.rsqrt(lax.optimization_barrier(jnp.mean(values * values, axis=-1, keepdims=True)) + EPS) * gain_in).astype(jnp.bfloat16)
    most = N_EP * N_TP * CAP
    blocks = FF // FF_DEV

    def one_expert(total, items):
        expert, gate_w, up_w, down_w = items
        hit = routes == expert
        chosen = jnp.any(hit, axis=1)
        index = jnp.nonzero(chosen, size=most, fill_value=0)[0].astype(jnp.int32)
        count = jnp.sum(chosen.astype(jnp.int32))
        live = (jnp.arange(most, dtype=jnp.int32) < count).astype(jnp.float32)
        rows = normed[index]
        gate = jnp.dot(rows, gate_w, preferred_element_type=jnp.float32)
        up = jnp.dot(rows, up_w, preferred_element_type=jnp.float32)
        hidden = (jax.nn.silu(gate) * up).astype(jnp.bfloat16)
        parts = jnp.einsum('rbf,bfd->brd', hidden.reshape(most, blocks, FF_DEV).astype(jnp.float32), down_w.reshape(blocks, FF_DEV, D).astype(jnp.float32))
        rounded = lax.optimization_barrier(parts.astype(jnp.bfloat16))
        summed = lax.optimization_barrier(jnp.sum(rounded.astype(jnp.float32), axis=0))
        result = lax.optimization_barrier(summed.astype(jnp.bfloat16)).astype(jnp.float32)
        weight = lax.optimization_barrier(jnp.sum(jnp.where(hit, gates, jnp.float32(0.0)), axis=1))[index] * live
        total = total.at[index].add(weight[:, None] * result)
        return (total, None)
    start = jnp.zeros((TOKENS, D), jnp.float32)
    combined, unused = lax.scan(one_expert, start, (jnp.arange(EXPERTS, dtype=jnp.int32), w_gate, w_up, w_down))
    scale = lax.rsqrt(lax.optimization_barrier(jnp.mean(combined * combined, axis=-1, keepdims=True)) + EPS)
    return (combined * scale * gain_out).astype(jnp.bfloat16)
```

```python
import functools

import jax
import jax.numpy as jnp
from jax import lax
from jax.experimental import pallas as pl
from jax.experimental.pallas import tpu as pltpu
from jax.sharding import PartitionSpec as P

EPS = 1e-06


def slot_table(routes, experts, capacity):
    sources, count, choose = routes.shape
    flat = routes.reshape(sources, count * choose)
    onehot = (flat[:, :, None] == jnp.arange(experts, dtype=jnp.int32)[None, None, :]).astype(
        jnp.int32
    )
    earlier = jnp.cumsum(onehot, axis=1) - onehot
    slot = jnp.sum(earlier * onehot, axis=2)
    return (flat * capacity + slot).reshape(sources, count, choose)


MESH = pl.DeviceIdType.MESH


def fused_kernel(
    experts,
    groups,
    capacity,
    tokens_hbm,
    gain_in_hbm,
    routes_hbm,
    gates_hbm,
    w_gate_hbm,
    w_up_hbm,
    w_down_hbm,
    gain_out_hbm,
    out_ref,
    tokens_ref,
    gain_in_ref,
    routes_ref,
    gates_ref,
    gain_out_ref,
    stage,
    table,
    w_gate,
    w_up,
    w_down,
    earlier_ref,
    picked,
    rows,
    hidden,
    part,
    pair_in,
    cross_out,
    cross_in,
    home_out,
    home,
    combined,
    squares,
    weight_sem,
    small_sem,
    d1_send,
    d1_recv,
    d2p_send,
    d2p_recv,
    d2x_send,
    d2x_recv,
    d3_send,
    d3_recv,
    r1_send,
    r1_recv,
    r2_send,
    r2_recv,
    r3_send,
    r3_recv,
    sq_send,
    sq_recv,
):
    z = lax.axis_index("ep")
    q = lax.axis_index("tp")
    core = lax.rem(q, 2)
    plane = q // 2
    partner = q + 1 - 2 * core
    across = lax.rem(q + 2, groups)
    count, width = tokens_ref.shape
    total = out_ref.shape[0]
    choose = routes_ref.shape[0]
    hidden_width = w_gate.shape[1]
    slice_width = out_ref.shape[1]
    block_rows = groups * capacity
    half_width = width // 2
    half_rows = block_rows // 2

    last = experts - 1
    side = z // 2
    inward = z + side * (last - 2 * z)
    near = [inward, 2 - 2 * inward, 1 + 2 * inward, last - inward]
    peer = [p + side * (last - 2 * p) for p in near]
    is_end = inward == 0

    small = [
        pltpu.make_async_copy(src, dst, small_sem.at[i])
        for i, (src, dst) in enumerate(
            (
                (tokens_hbm, tokens_ref),
                (routes_hbm, routes_ref),
                (gates_hbm, gates_ref),
                (gain_in_hbm, gain_in_ref),
                (gain_out_hbm, gain_out_ref),
            )
        )
    ]
    for copy in small:
        copy.start()
    weights = [
        pltpu.make_async_copy(src.at[0], dst, weight_sem.at[i])
        for i, (src, dst) in enumerate(
            ((w_gate_hbm, w_gate), (w_up_hbm, w_up), (w_down_hbm, w_down))
        )
    ]
    barrier = pltpu.get_barrier_semaphore()
    for step in range(1, experts):
        pl.semaphore_signal(
            barrier, inc=1, device_id={"ep": lax.rem(z + step, experts)}, device_id_type=MESH
        )
    for step in range(1, groups):
        pl.semaphore_signal(
            barrier, inc=1, device_id={"tp": lax.rem(q + step, groups)}, device_id_type=MESH
        )

    small[1].wait()
    small[2].wait()
    stage[...] = jnp.zeros_like(stage)
    stage[0:choose, :] = routes_ref[...].astype(jnp.float32)
    stage[choose : 2 * choose, :] = gates_ref[...]
    table[...] = jnp.transpose(stage[...])
    routes = table[:, 0:choose]
    lane = lax.broadcasted_iota(jnp.int32, (total, 128), 1).astype(jnp.float32)
    hit = ((routes[:, 0:1] == lane) | (routes[:, 1:2] == lane)).astype(jnp.float32)
    row_id = lax.broadcasted_iota(jnp.int32, (total, total), 0)
    col_id = lax.broadcasted_iota(jnp.int32, (total, total), 1)
    before = ((col_id < row_id) & (col_id // count == row_id // count)).astype(jnp.float32)
    earlier_ref[...] = jnp.dot(
        before.astype(jnp.bfloat16), hit.astype(jnp.bfloat16), preferred_element_type=jnp.float32
    )

    own = pl.ds(pl.multiple_of(q * count, count), count)
    own_routes = table[own, :]
    own_earlier = earlier_ref[own, :]
    own_lane = lax.broadcasted_iota(jnp.int32, (count, 128), 1).astype(jnp.float32)
    slots = lax.broadcasted_iota(jnp.int32, (count, experts * capacity), 1).astype(jnp.float32)
    select = jnp.zeros((count, experts * capacity), jnp.float32)
    for k in range(choose):
        expert = own_routes[:, k : k + 1]
        slot = jnp.sum(
            jnp.where(own_lane == expert, own_earlier, 0.0), axis=1, keepdims=True
        )
        select = jnp.where(slots == expert * capacity + slot, 1.0, select)

    small[0].wait()
    small[3].wait()
    values = tokens_ref[...].astype(jnp.float32)
    normed = (
        values
        * lax.rsqrt(jnp.mean(values * values, axis=-1, keepdims=True) + EPS)
        * gain_in_ref[...]
    ).astype(jnp.bfloat16)
    picked[...] = (
        lax.dot_general(
            select.astype(jnp.bfloat16),
            normed,
            (((0,), (0,)), ((), ())),
            preferred_element_type=jnp.float32,
        )
        .astype(jnp.bfloat16)
        .reshape(experts, capacity, width)
    )
    rows[z, q] = picked[z]

    pl.semaphore_wait(barrier, experts - 1 + groups - 1)

    sent = {}

    def remote(src, dst, send, recv, where):
        return pltpu.make_async_remote_copy(
            src_ref=src,
            dst_ref=dst,
            send_sem=send,
            recv_sem=recv,
            device_id=where,
            device_id_type=MESH,
        )

    def launch(make, *where):
        make(*where).start()
        sent[(make.__name__,) + where] = make

    def columns(h):
        return pl.ds(h * half_width, half_width)

    def lines(h):
        return pl.ds(h * half_rows, half_rows)

    def z_in(k, h, outward):
        there = peer[k]
        return remote(
            picked.at[there, :, columns(h)],
            rows.at[z if outward else there, q, :, columns(h)],
            d1_send.at[k, h],
            d1_recv.at[z if outward else there, h],
            {"ep": there},
        )

    def x_in(k, h):
        block = rows.at[peer[k], q, :, columns(h)]
        return remote(block, block, d2x_send.at[k, h], d2x_recv.at[k, h], {"tp": across})

    def pair_of(k, h):
        block = rows.at[peer[k], q, :, columns(h)]
        return remote(block, block, d2p_send.at[k, h], d2p_recv.at[k, h], {"tp": partner})

    def pair_across(k, h):
        block = rows.at[peer[k], across, :, columns(h)]
        return remote(block, block, d3_send.at[k, h], d3_recv.at[k, h], {"tp": partner})

    def spread(k, h):
        if k:
            z_in(k, h, False).wait_recv()
        launch(x_in, k, h)
        launch(pair_of, k, h)

    def relay(k, h):
        x_in(k, h).wait_recv()
        launch(pair_across, k, h)

    def pair_back(k, own_plane):
        there = plane if own_plane else 1 - plane
        return remote(
            part.at[k, there, 1 - core],
            pair_in.at[k, there],
            r1_send.at[k, own_plane],
            r1_recv.at[k, own_plane],
            {"tp": partner},
        )

    def x_back(k, h):
        return remote(
            cross_out.at[k, lines(h)],
            cross_in.at[k, lines(h)],
            r2_send.at[k, h],
            r2_recv.at[k, h],
            {"tp": across},
        )

    def z_back(k, h, outward):
        there = peer[k]
        where = z if outward else there
        return remote(
            home_out.at[k, lines(h)],
            home.at[where, lines(h)],
            r3_send.at[k, h],
            r3_recv.at[where, h],
            {"ep": there},
        )

    tile = 256
    tiles = hidden_width // tile

    def multiply(k, between):
        for h in range(2):
            pair_of(k, h).wait_recv()
            pair_across(k, h).wait_recv()
        x = rows[peer[k]].reshape(block_rows, width)
        for i in range(tiles):
            cols = pl.ds(i * tile, tile)
            gate = jnp.dot(x, w_gate[:, cols], preferred_element_type=jnp.float32)
            up = jnp.dot(x, w_up[:, cols], preferred_element_type=jnp.float32)
            hidden[:, cols] = (gate / (1.0 + jnp.exp(-gate)) * up).astype(jnp.bfloat16)
        for act in between:
            act()
        if k == 0:
            weights[2].wait()
        for own_plane in (0, 1):
            there = plane if own_plane else 1 - plane
            for c in range(2):
                cols = pl.ds(
                    pl.multiple_of((2 * there + c) * slice_width, slice_width), slice_width
                )
                product = jnp.dot(hidden[...], w_down[:, cols], preferred_element_type=jnp.float32)
                part[k, there, c] = product.astype(jnp.bfloat16)
            launch(pair_back, k, own_plane)

    def cross(k, h):
        other = 1 - plane
        if h == 0:
            pair_back(k, 0).wait_recv()
        cross_out[k, lines(h)] = (
            part[k, other, core, lines(h)].astype(jnp.float32)
            + pair_in[k, other, lines(h)].astype(jnp.float32)
        ).astype(jnp.bfloat16)
        launch(x_back, k, h)

    def give_back(k, h):
        if h == 0:
            pair_back(k, 1).wait_recv()
        x_back(k, h).wait_recv()
        result = (
            part[k, plane, core, lines(h)].astype(jnp.float32)
            + pair_in[k, plane, lines(h)].astype(jnp.float32)
            + cross_in[k, lines(h)].astype(jnp.float32)
        ).astype(jnp.bfloat16)
        if k == 0:
            home[z, lines(h)] = result
        else:
            home_out[k, lines(h)] = result
            launch(z_back, k, h, True)

    def join(k, h):
        z_back(k, h, False).wait_recv()

    def combine(k, first):
        if k:
            for h in range(2):
                join(k, h)
        e = peer[k]
        expert = e.astype(jnp.float32)
        mine = table[:, 0:choose] == expert
        lanes = lax.broadcasted_iota(jnp.int32, (total, 128), 1).astype(jnp.float32)
        slot = jnp.sum(jnp.where(lanes == expert, earlier_ref[...], 0.0), axis=1, keepdims=True)
        block = lax.broadcasted_iota(jnp.int32, (total, 1), 0) // count
        named = jnp.max(mine.astype(jnp.float32), axis=1, keepdims=True)
        target = jnp.where(
            named > 0.0, slot + (block * capacity).astype(jnp.float32), jnp.float32(-1.0)
        )
        weight = jnp.sum(jnp.where(mine, table[:, choose : 2 * choose], 0.0), axis=1, keepdims=True)
        place = lax.broadcasted_iota(jnp.int32, (total, block_rows), 1).astype(jnp.float32)
        pick = (place == target).astype(jnp.float32).astype(jnp.bfloat16)
        term = weight * jnp.dot(pick, home[e], preferred_element_type=jnp.float32)
        combined[...] = term if first else combined[...] + term

    def todo(act, *arguments, where=None):
        def run():
            if where is None:
                act(*arguments)
            else:
                pl.when(is_end if where == "end" else jnp.logical_not(is_end))(
                    lambda: act(*arguments)
                )

        return run

    def end(act, *arguments):
        return todo(act, *arguments, where="end")

    def middle(act, *arguments):
        return todo(act, *arguments, where="middle")

    def send(k):
        for h in range(2):
            launch(z_in, k, h, True)

    for h in range(2):
        spread(0, h)
    send(2)
    middle(send, 1)()
    middle(send, 3)()
    for copy in weights:
        copy.start()
    spread(1, 0)
    relay(0, 0)
    spread(1, 1)
    relay(0, 1)
    end(send, 1)()
    end(send, 3)()
    weights[0].wait()
    weights[1].wait()
    multiply(0, [todo(relay, 1, 0), end(spread, 2, 0)])
    middle(spread, 2, 0)()
    relay(1, 1)
    end(spread, 2, 1)()
    multiply(1, [middle(spread, 2, 1), end(relay, 2, 0)])
    middle(relay, 2, 0)()
    cross(1, 0)
    relay(2, 1)
    spread(3, 0)
    multiply(2, [todo(spread, 3, 1), todo(cross, 1, 1)])
    give_back(1, 0)
    cross(2, 0)
    cross(2, 1)
    relay(3, 0)
    relay(3, 1)
    multiply(3, [todo(give_back, 1, 1)])
    cross(3, 0)
    cross(3, 1)
    give_back(2, 0)
    cross(0, 0)
    cross(0, 1)
    give_back(2, 1)
    give_back(3, 0)
    give_back(3, 1)
    combine(2, True)
    combine(1, False)
    give_back(0, 0)
    give_back(0, 1)
    combine(0, False)
    combine(3, False)

    small[4].wait()
    value = combined[...]
    ones = jnp.ones((8, slice_width), jnp.float32)
    squares[q] = lax.dot_general(
        ones,
        value * value,
        (((1,), (1,)), ((), ())),
        preferred_element_type=jnp.float32,
        precision=lax.Precision.HIGHEST,
    )

    def share(step):
        return remote(
            squares.at[q],
            squares.at[q],
            sq_send.at[step],
            sq_recv.at[step],
            {"tp": lax.rem(q + step, groups)},
        )

    for step in range(1, groups):
        launch(share, step)
    for step in range(1, groups):
        share(step).wait_recv()
    summed = squares[0]
    for i in range(1, groups):
        summed = summed + squares[i]
    scale = lax.rsqrt(summed / width + EPS)
    column = jnp.transpose(scale)[:, 0:1]
    out_ref[...] = (combined[...] * column * gain_out_ref[...]).astype(jnp.bfloat16)
    for key, make in sent.items():
        make(*key[1:]).wait_send()


def fused(tokens, gain_in, routes, gates, w_gate, w_up, w_down, gain_out, capacity):
    experts = lax.axis_size("ep")
    groups = lax.axis_size("tp")
    count, width = tokens.shape
    total = routes.shape[0]
    hidden_width = w_gate.shape[2]
    slice_width = width // groups
    block_rows = groups * capacity
    bf16, f32 = jnp.bfloat16, jnp.float32
    vmem = pl.BlockSpec(memory_space=pltpu.VMEM)
    hbm = pl.BlockSpec(memory_space=pl.ANY)
    dma = pltpu.SemaphoreType.DMA
    return pl.pallas_call(
        functools.partial(fused_kernel, experts, groups, capacity),
        out_shape=jax.ShapeDtypeStruct((total, slice_width), bf16),
        in_specs=[hbm] * 8,
        out_specs=vmem,
        scratch_shapes=[
            pltpu.VMEM(tokens.shape, bf16),
            pltpu.VMEM((1, width), f32),
            pltpu.VMEM((routes.shape[1], total), jnp.int32),
            pltpu.VMEM((routes.shape[1], total), f32),
            pltpu.VMEM((1, slice_width), f32),
            pltpu.VMEM((8, total), f32),
            pltpu.VMEM((total, 8), f32),
            pltpu.VMEM((width, hidden_width), bf16),
            pltpu.VMEM((width, hidden_width), bf16),
            pltpu.VMEM((hidden_width, width), bf16),
            pltpu.VMEM((total, 128), f32),
            pltpu.VMEM((experts, capacity, width), bf16),
            pltpu.VMEM((experts, groups, capacity, width), bf16),
            pltpu.VMEM((block_rows, hidden_width), bf16),
            pltpu.VMEM((experts, groups // 2, 2, block_rows, slice_width), bf16),
            pltpu.VMEM((experts, groups // 2, block_rows, slice_width), bf16),
            pltpu.VMEM((experts, block_rows, slice_width), bf16),
            pltpu.VMEM((experts, block_rows, slice_width), bf16),
            pltpu.VMEM((experts, block_rows, slice_width), bf16),
            pltpu.VMEM((experts, block_rows, slice_width), bf16),
            pltpu.VMEM((total, slice_width), f32),
            pltpu.VMEM((groups, 8, total), f32),
            dma((3,)),
            dma((5,)),
        ]
        + [dma((experts, 2)) for _ in range(14)]
        + [dma((groups,)) for _ in range(2)],
        compiler_params=pltpu.CompilerParams(
            collective_id=0, has_side_effects=True, vmem_limit_bytes=60 * 1024 * 1024
        ),
    )(tokens, gain_in[None], routes.T, gates.T, w_gate, w_up, w_down, gain_out[None])


def local(tokens, gain_in, routes, gates, w_gate, w_up, w_down, gain_out):
    count, width = tokens.shape
    choose = routes.shape[1]
    experts = lax.axis_size("ep")
    groups = lax.axis_size("tp")
    capacity = (3 * count * choose + 2 * experts - 1) // (2 * experts)
    hidden_width = w_gate.shape[2]
    if experts == 4 and groups == 4 and choose == 2 and capacity % 16 == 0 and hidden_width % 256 == 0:
        return fused(
            tokens, gain_in, routes, gates, w_gate, w_up, w_down, gain_out, capacity
        )
    values = tokens.astype(jnp.float32)
    normed = (
        values * lax.rsqrt(jnp.mean(values * values, axis=-1, keepdims=True) + EPS) * gain_in
    ).astype(jnp.bfloat16)
    positions = slot_table(routes.reshape(groups, count, choose), experts, capacity)
    own = lax.dynamic_index_in_dim(positions, lax.axis_index("tp"), 0, keepdims=False)
    slots = jnp.arange(experts * capacity, dtype=jnp.int32)
    select = jnp.sum((own[None, :, :] == slots[:, None, None]).astype(jnp.bfloat16), axis=2)
    outgoing = jnp.dot(select, normed, preferred_element_type=jnp.float32).astype(jnp.bfloat16)
    outgoing = outgoing.reshape(experts, capacity, width)
    arrived = lax.all_to_all(outgoing, "ep", split_axis=0, concat_axis=0, tiled=True)
    piece = lax.all_gather(arrived[:, None], "tp", axis=1, tiled=True)
    flat = piece.reshape(-1, width)
    gate = jnp.dot(flat, w_gate[0], preferred_element_type=jnp.float32)
    up = jnp.dot(flat, w_up[0], preferred_element_type=jnp.float32)
    hidden = (jax.nn.silu(gate) * up).astype(jnp.bfloat16)
    hidden = hidden.reshape(piece.shape[:-1] + (hidden_width,))
    partial_value = jnp.dot(
        hidden.reshape(-1, hidden_width), w_down[0], preferred_element_type=jnp.float32
    )
    summed = lax.psum_scatter(
        partial_value.astype(jnp.bfloat16), "tp", scatter_dimension=1, tiled=True
    )
    slice_width = width // groups
    expert_out = summed.reshape(experts, groups * capacity, slice_width)
    returned = lax.all_to_all(expert_out, "ep", split_axis=0, concat_axis=0, tiled=True)
    returned = returned.reshape(experts, groups, capacity, slice_width).transpose(1, 0, 2, 3)
    returned = returned.reshape(groups, experts * capacity, slice_width).astype(jnp.float32)
    weights = gates.reshape(groups, count, choose)
    combine = jnp.sum(
        jnp.where(
            positions[..., None] == slots[None, None, None, :], weights[..., None], jnp.float32(0.0)
        ),
        axis=2,
    )
    combined = jnp.einsum("gtp,gpd->gtd", combine, returned, precision=lax.Precision.HIGHEST)
    combined = combined.reshape(groups * count, slice_width)
    squares = lax.psum(jnp.sum(combined * combined, axis=1), "tp")
    scale = lax.rsqrt(squares / width + EPS)
    return (combined * scale[:, None] * gain_out).astype(jnp.bfloat16)


def solution(mesh):
    in_specs = (
        P(("grp", "ep", "tp"), None),
        P(),
        P(("grp", "ep"), None),
        P(("grp", "ep"), None),
        P("ep", None, "tp"),
        P("ep", None, "tp"),
        P("ep", "tp", None),
        P("tp"),
    )
    out_specs = P(("grp", "ep"), "tp")
    return jax.shard_map(local, mesh=mesh, in_specs=in_specs, out_specs=out_specs, check_vma=False)
```

```python
import functools

import jax
import jax.numpy as jnp
from jax import lax
from jax.experimental import pallas as pl
from jax.experimental.pallas import tpu as pltpu
from jax.sharding import PartitionSpec as P

EPS = 1e-06


def slot_table(routes, experts, capacity):
    sources, count, choose = routes.shape
    flat = routes.reshape(sources, count * choose)
    onehot = (flat[:, :, None] == jnp.arange(experts, dtype=jnp.int32)[None, None, :]).astype(
        jnp.int32
    )
    earlier = jnp.cumsum(onehot, axis=1) - onehot
    slot = jnp.sum(earlier * onehot, axis=2)
    return (flat * capacity + slot).reshape(sources, count, choose)


MESH = pl.DeviceIdType.MESH


def fused_kernel(
    experts,
    groups,
    capacity,
    tokens_hbm,
    gain_in_hbm,
    routes_hbm,
    gates_hbm,
    w_gate_hbm,
    w_up_hbm,
    w_down_hbm,
    gain_out_hbm,
    out_ref,
    tokens_ref,
    gain_in_ref,
    routes_ref,
    gates_ref,
    gain_out_ref,
    stage,
    table,
    w_gate,
    w_up,
    w_down,
    earlier_ref,
    picked,
    rows,
    hidden,
    part,
    pair_in,
    cross_out,
    cross_in,
    home_out,
    home,
    combined,
    squares,
    weight_sem,
    small_sem,
    d1_send,
    d1_recv,
    d2p_send,
    d2p_recv,
    d2x_send,
    d2x_recv,
    d3_send,
    d3_recv,
    r1_send,
    r1_recv,
    r2_send,
    r2_recv,
    r3_send,
    r3_recv,
    sq_send,
    sq_recv,
):
    z = lax.axis_index("ep")
    q = lax.axis_index("tp")
    core = lax.rem(q, 2)
    plane = q // 2
    partner = q + 1 - 2 * core
    across = lax.rem(q + 2, groups)
    count, width = tokens_ref.shape
    total = out_ref.shape[0]
    choose = routes_ref.shape[0]
    hidden_width = w_gate.shape[1]
    slice_width = out_ref.shape[1]
    block_rows = groups * capacity
    pieces = d1_recv.shape[1]
    per_half = pieces // 2
    piece_width = width // pieces
    piece_rows = block_rows // pieces

    last = experts - 1
    side = z // 2
    inward = z + side * (last - 2 * z)
    near = [inward, 2 - 2 * inward, 1 + inward, last + 0 * inward]
    peer = [p + side * (last - 2 * p) for p in near]
    is_end = inward == 0

    small = [
        pltpu.make_async_copy(src, dst, small_sem.at[i])
        for i, (src, dst) in enumerate(
            (
                (tokens_hbm, tokens_ref),
                (routes_hbm, routes_ref),
                (gates_hbm, gates_ref),
                (gain_in_hbm, gain_in_ref),
                (gain_out_hbm, gain_out_ref),
            )
        )
    ]
    for copy in small:
        copy.start()
    weights = [
        pltpu.make_async_copy(src.at[0], dst, weight_sem.at[i])
        for i, (src, dst) in enumerate(
            ((w_gate_hbm, w_gate), (w_up_hbm, w_up), (w_down_hbm, w_down))
        )
    ]
    barrier = pltpu.get_barrier_semaphore()
    for step in range(1, experts):
        pl.semaphore_signal(
            barrier, inc=1, device_id={"ep": lax.rem(z + step, experts)}, device_id_type=MESH
        )
    for step in range(1, groups):
        pl.semaphore_signal(
            barrier, inc=1, device_id={"tp": lax.rem(q + step, groups)}, device_id_type=MESH
        )

    small[1].wait()
    small[2].wait()
    stage[...] = jnp.zeros_like(stage)
    stage[0:choose, :] = routes_ref[...].astype(jnp.float32)
    stage[choose : 2 * choose, :] = gates_ref[...]
    table[...] = jnp.transpose(stage[...])
    own = pl.ds(pl.multiple_of(q * count, count), count)
    own_routes = table[own, :]
    own_lane = lax.broadcasted_iota(jnp.int32, (count, 128), 1).astype(jnp.float32)
    own_hit = (own_routes[:, 0:1] == own_lane) | (own_routes[:, 1:2] == own_lane)
    own_row = lax.broadcasted_iota(jnp.int32, (count, count), 0)
    own_col = lax.broadcasted_iota(jnp.int32, (count, count), 1)
    own_earlier = jnp.dot(
        (own_col < own_row).astype(jnp.float32).astype(jnp.bfloat16),
        own_hit.astype(jnp.float32).astype(jnp.bfloat16),
        preferred_element_type=jnp.float32,
    )
    slots = lax.broadcasted_iota(jnp.int32, (count, experts * capacity), 1).astype(jnp.float32)
    select = jnp.zeros((count, experts * capacity), jnp.float32)
    for k in range(choose):
        expert = own_routes[:, k : k + 1]
        slot = jnp.sum(
            jnp.where(own_lane == expert, own_earlier, 0.0), axis=1, keepdims=True
        )
        select = jnp.where(slots == expert * capacity + slot, 1.0, select)

    small[0].wait()
    small[3].wait()
    values = tokens_ref[...].astype(jnp.float32)
    normed = (
        values
        * lax.rsqrt(jnp.mean(values * values, axis=-1, keepdims=True) + EPS)
        * gain_in_ref[...]
    ).astype(jnp.bfloat16)
    picked[...] = (
        lax.dot_general(
            select.astype(jnp.bfloat16),
            normed,
            (((0,), (0,)), ((), ())),
            preferred_element_type=jnp.float32,
        )
        .astype(jnp.bfloat16)
        .reshape(experts, capacity, width)
    )
    rows[z, q] = picked[z]

    pl.semaphore_wait(barrier, experts - 1 + groups - 1)

    def remote(src, dst, send, recv, where):
        return pltpu.make_async_remote_copy(
            src_ref=src,
            dst_ref=dst,
            send_sem=send,
            recv_sem=recv,
            device_id=where,
            device_id_type=MESH,
        )

    def columns(h):
        return pl.ds(h * piece_width, piece_width)

    def lines(h):
        return pl.ds(h * piece_rows, piece_rows)

    def in_half(half):
        return range(half * per_half, (half + 1) * per_half)

    def z_in(k, h, outward):
        there = peer[k]
        where = z if outward else there
        return remote(
            picked.at[there, :, columns(h)],
            rows.at[where, q, :, columns(h)],
            d1_send.at[0],
            d1_recv.at[where, h],
            {"ep": there},
        )

    def x_in(k, h):
        block = rows.at[peer[k], q, :, columns(h)]
        return remote(block, block, d2x_send.at[0], d2x_recv.at[k, h], {"tp": across})

    def pair_of(k, cols):
        block = rows.at[peer[k], q, :, cols]
        return remote(block, block, d2p_send.at[0], d2p_recv.at[k], {"tp": partner})

    def pair_across(k, cols):
        block = rows.at[peer[k], across, :, cols]
        return remote(block, block, d3_send.at[0], d3_recv.at[k], {"tp": partner})

    def spread(k, half):
        for h in in_half(half):
            if k:
                z_in(k, h, False).wait_recv()
            x_in(k, h).start()
            pair_of(k, columns(h)).start()

    def relay(k, half):
        for h in in_half(half):
            x_in(k, h).wait_recv()
            pair_across(k, columns(h)).start()

    def pair_back(k, own_plane):
        there = plane if own_plane else 1 - plane
        return remote(
            part.at[k, there, 1 - core],
            pair_in.at[k, there],
            r1_send.at[0],
            r1_recv.at[k, own_plane],
            {"tp": partner},
        )

    def x_back(k, h):
        return remote(
            cross_out.at[k, lines(h)],
            cross_in.at[k, lines(h)],
            r2_send.at[0],
            r2_recv.at[k, h],
            {"tp": across},
        )

    def z_back(k, rows_of, outward):
        there = peer[k]
        where = z if outward else there
        return remote(
            home_out.at[k, rows_of],
            home.at[where, rows_of],
            r3_send.at[0],
            r3_recv.at[where],
            {"ep": there},
        )

    tile = 256
    tiles = hidden_width // tile

    def multiply(k, between):
        every = pl.ds(0, width)
        pair_of(k, every).wait_recv()
        pair_across(k, every).wait_recv()
        x = rows[peer[k]].reshape(block_rows, width)
        for i in range(tiles):
            cols = pl.ds(i * tile, tile)
            gate = jnp.dot(x, w_gate[:, cols], preferred_element_type=jnp.float32)
            up = jnp.dot(x, w_up[:, cols], preferred_element_type=jnp.float32)
            hidden[:, cols] = (gate / (1.0 + jnp.exp(-gate)) * up).astype(jnp.bfloat16)
        for act in between:
            act()
        if k == 0:
            weights[2].wait()
        for own_plane in (0, 1):
            there = plane if own_plane else 1 - plane
            for c in range(2):
                cols = pl.ds(
                    pl.multiple_of((2 * there + c) * slice_width, slice_width), slice_width
                )
                product = jnp.dot(hidden[...], w_down[:, cols], preferred_element_type=jnp.float32)
                part[k, there, c] = product.astype(jnp.bfloat16)
            pair_back(k, own_plane).start()

    def cross(k, half):
        other = 1 - plane
        if half == 0:
            pair_back(k, 0).wait_recv()
        for h in in_half(half):
            cross_out[k, lines(h)] = (
                part[k, other, core, lines(h)].astype(jnp.float32)
                + pair_in[k, other, lines(h)].astype(jnp.float32)
            ).astype(jnp.bfloat16)
            x_back(k, h).start()

    def give_back(k, half):
        if half == 0:
            pair_back(k, 1).wait_recv()
        for h in in_half(half):
            x_back(k, h).wait_recv()
            result = (
                part[k, plane, core, lines(h)].astype(jnp.float32)
                + pair_in[k, plane, lines(h)].astype(jnp.float32)
                + cross_in[k, lines(h)].astype(jnp.float32)
            ).astype(jnp.bfloat16)
            if k == 0:
                home[z, lines(h)] = result
            else:
                home_out[k, lines(h)] = result
                z_back(k, lines(h), True).start()

    def count_earlier():
        routes = table[:, 0:choose]
        lane = lax.broadcasted_iota(jnp.int32, (total, 128), 1).astype(jnp.float32)
        hit = ((routes[:, 0:1] == lane) | (routes[:, 1:2] == lane)).astype(jnp.float32)
        row_id = lax.broadcasted_iota(jnp.int32, (total, total), 0)
        col_id = lax.broadcasted_iota(jnp.int32, (total, total), 1)
        before = ((col_id < row_id) & (col_id // count == row_id // count)).astype(jnp.float32)
        earlier_ref[...] = jnp.dot(
            before.astype(jnp.bfloat16),
            hit.astype(jnp.bfloat16),
            preferred_element_type=jnp.float32,
        )

    def join(k):
        z_back(k, pl.ds(0, block_rows), False).wait_recv()

    def combine(k, first):
        if k:
            join(k)
        e = peer[k]
        expert = e.astype(jnp.float32)
        mine = table[:, 0:choose] == expert
        lanes = lax.broadcasted_iota(jnp.int32, (total, 128), 1).astype(jnp.float32)
        slot = jnp.sum(jnp.where(lanes == expert, earlier_ref[...], 0.0), axis=1, keepdims=True)
        block = lax.broadcasted_iota(jnp.int32, (total, 1), 0) // count
        named = jnp.max(mine.astype(jnp.float32), axis=1, keepdims=True)
        target = jnp.where(
            named > 0.0, slot + (block * capacity).astype(jnp.float32), jnp.float32(-1.0)
        )
        weight = jnp.sum(jnp.where(mine, table[:, choose : 2 * choose], 0.0), axis=1, keepdims=True)
        place = lax.broadcasted_iota(jnp.int32, (total, block_rows), 1).astype(jnp.float32)
        pick = (place == target).astype(jnp.float32).astype(jnp.bfloat16)
        term = weight * jnp.dot(pick, home[e], preferred_element_type=jnp.float32)
        combined[...] = term if first else combined[...] + term

    def todo(act, *arguments, where=None):
        def run():
            if where is None:
                act(*arguments)
            else:
                pl.when(is_end if where == "end" else jnp.logical_not(is_end))(
                    lambda: act(*arguments)
                )

        return run

    def end(act, *arguments):
        return todo(act, *arguments, where="end")

    def middle(act, *arguments):
        return todo(act, *arguments, where="middle")

    def send(k):
        for h in range(pieces):
            z_in(k, h, True).start()

    for h in range(2):
        spread(0, h)
    end(send, 2)()
    middle(send, 3)()
    middle(send, 1)()
    middle(send, 2)()
    for copy in weights:
        copy.start()
    count_earlier()
    spread(1, 0)
    relay(0, 0)
    spread(1, 1)
    relay(0, 1)
    weights[0].wait()
    weights[1].wait()
    multiply(0, [end(send, 1), end(send, 3), todo(spread, 2, 0)])
    relay(1, 0)
    relay(1, 1)
    spread(2, 1)
    cross(0, 0)
    multiply(1, [todo(relay, 2, 0)])
    relay(2, 1)
    cross(1, 0)
    end(cross, 1, 1)()
    middle(spread, 3, 0)()
    multiply(2, [middle(spread, 3, 1)])
    end(spread, 3, 0)()
    end(give_back, 1, 0)()
    end(spread, 3, 1)()
    end(give_back, 1, 1)()
    middle(cross, 1, 1)()
    cross(2, 0)
    cross(2, 1)
    middle(give_back, 1, 0)()
    relay(3, 0)
    relay(3, 1)
    multiply(3, [end(give_back, 2, 0), middle(give_back, 1, 1)])
    cross(3, 0)
    cross(3, 1)
    middle(give_back, 2, 0)()
    give_back(2, 1)
    cross(0, 1)
    give_back(3, 0)
    give_back(3, 1)
    combine(2, True)
    give_back(0, 0)
    give_back(0, 1)
    combine(0, False)
    combine(1, False)
    combine(3, False)

    small[4].wait()
    value = combined[...]
    folded = sum(
        value[:, i : i + 128] * value[:, i : i + 128] for i in range(0, slice_width, 128)
    )
    ones = jnp.ones((8, 128), jnp.float32)
    squares[q] = lax.dot_general(
        ones,
        folded,
        (((1,), (1,)), ((), ())),
        preferred_element_type=jnp.float32,
        precision=lax.Precision.HIGHEST,
    )

    def share(step, rows_of):
        return remote(
            squares.at[rows_of],
            squares.at[rows_of],
            sq_send.at[0],
            sq_recv.at[step],
            {"tp": lax.rem(q + step, groups)},
        )

    for step in range(1, groups):
        share(step, pl.ds(q, 1)).start()
    for step in range(1, groups):
        share(step, pl.ds(q, 1)).wait_recv()
    summed = squares[0]
    for i in range(1, groups):
        summed = summed + squares[i]
    scale = lax.rsqrt(summed / width + EPS)
    column = jnp.transpose(scale)[:, 0:1]
    out_ref[...] = (combined[...] * column * gain_out_ref[...]).astype(jnp.bfloat16)

    def drain(block, semaphore):
        remote(block, block, semaphore.at[0], semaphore.at[0], {"tp": across}).wait_send()

    drain(picked.at[0 : experts - 1], d1_send)
    drain(rows.at[0], d2x_send)
    drain(rows.at[0], d2p_send)
    drain(rows.at[0], d3_send)
    drain(pair_in, r1_send)
    drain(cross_out, r2_send)
    drain(home_out.at[1:experts], r3_send)
    drain(squares.at[1:groups], sq_send)


def fused(tokens, gain_in, routes, gates, w_gate, w_up, w_down, gain_out, capacity):
    experts = lax.axis_size("ep")
    groups = lax.axis_size("tp")
    count, width = tokens.shape
    total = routes.shape[0]
    hidden_width = w_gate.shape[2]
    slice_width = width // groups
    block_rows = groups * capacity
    bf16, f32 = jnp.bfloat16, jnp.float32
    vmem = pl.BlockSpec(memory_space=pltpu.VMEM)
    hbm = pl.BlockSpec(memory_space=pl.ANY)
    dma = pltpu.SemaphoreType.DMA
    return pl.pallas_call(
        functools.partial(fused_kernel, experts, groups, capacity),
        out_shape=jax.ShapeDtypeStruct((total, slice_width), bf16),
        in_specs=[hbm] * 8,
        out_specs=vmem,
        scratch_shapes=[
            pltpu.VMEM(tokens.shape, bf16),
            pltpu.VMEM((1, width), f32),
            pltpu.VMEM((routes.shape[1], total), jnp.int32),
            pltpu.VMEM((routes.shape[1], total), f32),
            pltpu.VMEM((1, slice_width), f32),
            pltpu.VMEM((8, total), f32),
            pltpu.VMEM((total, 8), f32),
            pltpu.VMEM((width, hidden_width), bf16),
            pltpu.VMEM((width, hidden_width), bf16),
            pltpu.VMEM((hidden_width, width), bf16),
            pltpu.VMEM((total, 128), f32),
            pltpu.VMEM((experts, capacity, width), bf16),
            pltpu.VMEM((experts, groups, capacity, width), bf16),
            pltpu.VMEM((block_rows, hidden_width), bf16),
            pltpu.VMEM((experts, groups // 2, 2, block_rows, slice_width), bf16),
            pltpu.VMEM((experts, groups // 2, block_rows, slice_width), bf16),
            pltpu.VMEM((experts, block_rows, slice_width), bf16),
            pltpu.VMEM((experts, block_rows, slice_width), bf16),
            pltpu.VMEM((experts, block_rows, slice_width), bf16),
            pltpu.VMEM((experts, block_rows, slice_width), bf16),
            pltpu.VMEM((total, slice_width), f32),
            pltpu.VMEM((groups, 8, total), f32),
            dma((3,)),
            dma((5,)),
            dma((1,)),
            dma((experts, 4)),
            dma((1,)),
            dma((experts,)),
            dma((1,)),
            dma((experts, 4)),
            dma((1,)),
            dma((experts,)),
            dma((1,)),
            dma((experts, 2)),
            dma((1,)),
            dma((experts, 4)),
            dma((1,)),
            dma((experts,)),
            dma((1,)),
            dma((groups,)),
        ],
        compiler_params=pltpu.CompilerParams(
            collective_id=0, has_side_effects=True, vmem_limit_bytes=48000 * 1024
        ),
    )(
        *(
            pltpu.with_memory_space_constraint(array, pltpu.HBM)
            for array in (
                tokens,
                gain_in[None],
                routes.T,
                gates.T,
                w_gate,
                w_up,
                w_down,
                gain_out[None],
            )
        )
    )


def local(tokens, gain_in, routes, gates, w_gate, w_up, w_down, gain_out):
    count, width = tokens.shape
    choose = routes.shape[1]
    experts = lax.axis_size("ep")
    groups = lax.axis_size("tp")
    capacity = (3 * count * choose + 2 * experts - 1) // (2 * experts)
    hidden_width = w_gate.shape[2]
    if experts == 4 and groups == 4 and choose == 2 and capacity % 16 == 0 and hidden_width % 256 == 0:
        return fused(
            tokens, gain_in, routes, gates, w_gate, w_up, w_down, gain_out, capacity
        )
    values = tokens.astype(jnp.float32)
    normed = (
        values * lax.rsqrt(jnp.mean(values * values, axis=-1, keepdims=True) + EPS) * gain_in
    ).astype(jnp.bfloat16)
    positions = slot_table(routes.reshape(groups, count, choose), experts, capacity)
    own = lax.dynamic_index_in_dim(positions, lax.axis_index("tp"), 0, keepdims=False)
    slots = jnp.arange(experts * capacity, dtype=jnp.int32)
    select = jnp.sum((own[None, :, :] == slots[:, None, None]).astype(jnp.bfloat16), axis=2)
    outgoing = jnp.dot(select, normed, preferred_element_type=jnp.float32).astype(jnp.bfloat16)
    outgoing = outgoing.reshape(experts, capacity, width)
    arrived = lax.all_to_all(outgoing, "ep", split_axis=0, concat_axis=0, tiled=True)
    piece = lax.all_gather(arrived[:, None], "tp", axis=1, tiled=True)
    flat = piece.reshape(-1, width)
    gate = jnp.dot(flat, w_gate[0], preferred_element_type=jnp.float32)
    up = jnp.dot(flat, w_up[0], preferred_element_type=jnp.float32)
    hidden = (jax.nn.silu(gate) * up).astype(jnp.bfloat16)
    hidden = hidden.reshape(piece.shape[:-1] + (hidden_width,))
    partial_value = jnp.dot(
        hidden.reshape(-1, hidden_width), w_down[0], preferred_element_type=jnp.float32
    )
    summed = lax.psum_scatter(
        partial_value.astype(jnp.bfloat16), "tp", scatter_dimension=1, tiled=True
    )
    slice_width = width // groups
    expert_out = summed.reshape(experts, groups * capacity, slice_width)
    returned = lax.all_to_all(expert_out, "ep", split_axis=0, concat_axis=0, tiled=True)
    returned = returned.reshape(experts, groups, capacity, slice_width).transpose(1, 0, 2, 3)
    returned = returned.reshape(groups, experts * capacity, slice_width).astype(jnp.float32)
    weights = gates.reshape(groups, count, choose)
    combine = jnp.sum(
        jnp.where(
            positions[..., None] == slots[None, None, None, :], weights[..., None], jnp.float32(0.0)
        ),
        axis=2,
    )
    combined = jnp.einsum("gtp,gpd->gtd", combine, returned, precision=lax.Precision.HIGHEST)
    combined = combined.reshape(groups * count, slice_width)
    squares = lax.psum(jnp.sum(combined * combined, axis=1), "tp")
    scale = lax.rsqrt(squares / width + EPS)
    return (combined * scale[:, None] * gain_out).astype(jnp.bfloat16)


def solution(mesh):
    in_specs = (
        P(("grp", "ep", "tp"), None),
        P(),
        P(("grp", "ep"), None),
        P(("grp", "ep"), None),
        P("ep", None, "tp"),
        P("ep", None, "tp"),
        P("ep", "tp", None),
        P("tp"),
    )
    out_specs = P(("grp", "ep"), "tp")
    return jax.shard_map(local, mesh=mesh, in_specs=in_specs, out_specs=out_specs, check_vma=False)
```

```python
import functools

import jax
import jax.numpy as jnp
from jax import lax
from jax.experimental import pallas as pl
from jax.experimental.pallas import tpu as pltpu
from jax.sharding import PartitionSpec as P

EPS = 1e-06


def slot_table(routes, experts, capacity):
    sources, count, choose = routes.shape
    flat = routes.reshape(sources, count * choose)
    onehot = (flat[:, :, None] == jnp.arange(experts, dtype=jnp.int32)[None, None, :]).astype(
        jnp.int32
    )
    earlier = jnp.cumsum(onehot, axis=1) - onehot
    slot = jnp.sum(earlier * onehot, axis=2)
    return (flat * capacity + slot).reshape(sources, count, choose)


MESH = pl.DeviceIdType.MESH


def fused_kernel(
    experts,
    groups,
    capacity,
    tokens_hbm,
    gain_in_hbm,
    routes_hbm,
    gates_hbm,
    w_gate_hbm,
    w_up_hbm,
    w_down_hbm,
    gain_out_hbm,
    out_ref,
    tokens_ref,
    gain_in_ref,
    routes_ref,
    gates_ref,
    gain_out_ref,
    stage,
    table,
    w_gate,
    w_up,
    w_down,
    earlier_ref,
    picked,
    rows,
    hidden,
    part,
    pair_in,
    cross_out,
    cross_in,
    home_out,
    home,
    combined,
    gate_sum,
    up_sum,
    squares,
    weight_sem,
    small_sem,
    d1_send,
    d1_recv,
    d2p_send,
    d2p_recv,
    d2x_send,
    d2x_recv,
    d3_send,
    d3_recv,
    r1_send,
    r1_recv,
    r2_send,
    r2_recv,
    r3_send,
    r3_recv,
    sq_send,
    sq_recv,
):
    z = lax.axis_index("ep")
    q = lax.axis_index("tp")
    core = lax.rem(q, 2)
    plane = q // 2
    partner = q + 1 - 2 * core
    across = lax.rem(q + 2, groups)
    count, width = tokens_ref.shape
    total = out_ref.shape[0]
    choose = routes_ref.shape[0]
    hidden_width = w_gate.shape[1]
    slice_width = out_ref.shape[1]
    block_rows = groups * capacity
    pieces = d1_recv.shape[1]
    per_half = pieces // 2
    piece_width = width // pieces
    piece_rows = block_rows // pieces

    last = experts - 1
    side = z // 2
    inward = z + side * (last - 2 * z)
    near = [inward, 2 - 2 * inward, 1 + inward, last + 0 * inward]
    peer = [p + side * (last - 2 * p) for p in near]
    is_end = inward == 0

    small = [
        pltpu.make_async_copy(src, dst, small_sem.at[i])
        for i, (src, dst) in enumerate(
            (
                (tokens_hbm, tokens_ref),
                (routes_hbm, routes_ref),
                (gates_hbm, gates_ref),
                (gain_in_hbm, gain_in_ref),
                (gain_out_hbm, gain_out_ref),
            )
        )
    ]
    for copy in small:
        copy.start()
    weights = [
        pltpu.make_async_copy(src.at[0], dst, weight_sem.at[i])
        for i, (src, dst) in enumerate(
            ((w_gate_hbm, w_gate), (w_up_hbm, w_up), (w_down_hbm, w_down))
        )
    ]
    barrier = pltpu.get_barrier_semaphore()
    for step in range(1, experts):
        pl.semaphore_signal(
            barrier, inc=1, device_id={"ep": lax.rem(z + step, experts)}, device_id_type=MESH
        )
    for step in range(1, groups):
        pl.semaphore_signal(
            barrier, inc=1, device_id={"tp": lax.rem(q + step, groups)}, device_id_type=MESH
        )

    for i in (1, 2, 0, 3):
        small[i].wait()
    stage[...] = jnp.zeros_like(stage)
    stage[0:choose, :] = routes_ref[...].astype(jnp.float32)
    stage[choose : 2 * choose, :] = gates_ref[...]
    table[...] = jnp.transpose(stage[...])
    own = pl.ds(pl.multiple_of(q * count, count), count)
    own_routes = table[own, :]
    own_lane = lax.broadcasted_iota(jnp.int32, (count, 128), 1).astype(jnp.float32)
    own_hit = (own_routes[:, 0:1] == own_lane) | (own_routes[:, 1:2] == own_lane)
    own_row = lax.broadcasted_iota(jnp.int32, (count, count), 0)
    own_col = lax.broadcasted_iota(jnp.int32, (count, count), 1)
    own_earlier = jnp.dot(
        (own_col < own_row).astype(jnp.float32).astype(jnp.bfloat16),
        own_hit.astype(jnp.float32).astype(jnp.bfloat16),
        preferred_element_type=jnp.float32,
    )
    slots = lax.broadcasted_iota(jnp.int32, (count, experts * capacity), 1).astype(jnp.float32)
    select = jnp.zeros((count, experts * capacity), jnp.float32)
    for k in range(choose):
        expert = own_routes[:, k : k + 1]
        slot = jnp.sum(
            jnp.where(own_lane == expert, own_earlier, 0.0), axis=1, keepdims=True
        )
        select = jnp.where(slots == expert * capacity + slot, 1.0, select)

    values = tokens_ref[...].astype(jnp.float32)
    normed = (
        values
        * lax.rsqrt(jnp.mean(values * values, axis=-1, keepdims=True) + EPS)
        * gain_in_ref[...]
    ).astype(jnp.bfloat16)
    picked[...] = (
        lax.dot_general(
            select.astype(jnp.bfloat16),
            normed,
            (((0,), (0,)), ((), ())),
            preferred_element_type=jnp.float32,
        )
        .astype(jnp.bfloat16)
        .reshape(experts, capacity, width)
    )
    rows[z, q] = picked[z]

    pl.semaphore_wait(barrier, experts - 1 + groups - 1)

    def remote(src, dst, send, recv, where):
        return pltpu.make_async_remote_copy(
            src_ref=src,
            dst_ref=dst,
            send_sem=send,
            recv_sem=recv,
            device_id=where,
            device_id_type=MESH,
        )

    def columns(h):
        return pl.ds(h * piece_width, piece_width)

    def lines(h):
        return pl.ds(h * piece_rows, piece_rows)

    def in_half(half):
        return range(half * per_half, (half + 1) * per_half)

    def z_in(k, h, outward):
        there = peer[k]
        where = z if outward else there
        return remote(
            picked.at[there, :, columns(h)],
            rows.at[where, q, :, columns(h)],
            d1_send.at[0],
            d1_recv.at[where, h],
            {"ep": there},
        )

    def x_in(k, h):
        block = rows.at[peer[k], q, :, columns(h)]
        return remote(block, block, d2x_send.at[0], d2x_recv.at[k, h], {"tp": across})

    def pair_of(k, cols, h):
        block = rows.at[peer[k], q, :, cols]
        return remote(block, block, d2p_send.at[0], d2p_recv.at[k, h // per_half], {"tp": partner})

    def pair_across(k, cols, h):
        block = rows.at[peer[k], across, :, cols]
        return remote(block, block, d3_send.at[0], d3_recv.at[k, h // per_half], {"tp": partner})

    def spread(k, half):
        for h in in_half(half):
            if k:
                z_in(k, h, False).wait_recv()
            x_in(k, h).start()
            pair_of(k, columns(h), h).start()

    def relay(k, half):
        for h in in_half(half):
            x_in(k, h).wait_recv()
            pair_across(k, columns(h), h).start()

    def pair_back(k, own_plane):
        there = plane if own_plane else 1 - plane
        return remote(
            part.at[k, there, 1 - core],
            pair_in.at[k, there],
            r1_send.at[0],
            r1_recv.at[k, own_plane],
            {"tp": partner},
        )

    def x_back(k, h):
        return remote(
            cross_out.at[k, lines(h)],
            cross_in.at[k, lines(h)],
            r2_send.at[0],
            r2_recv.at[k, h],
            {"tp": across},
        )

    def z_back(k, rows_of, outward):
        there = peer[k]
        where = z if outward else there
        return remote(
            home_out.at[k, rows_of],
            home.at[where, rows_of],
            r3_send.at[0],
            r3_recv.at[where],
            {"ep": there},
        )

    tile = 256
    tiles = hidden_width // tile

    half_width = width // 2

    def landed(k, half):
        cols = pl.ds(half * half_width, half_width)
        pair_of(k, cols, half * per_half).wait_recv()
        pair_across(k, cols, half * per_half).wait_recv()

    def begin(k):
        landed(k, 0)
        x = rows[peer[k], :, :, 0:half_width].reshape(block_rows, half_width)
        for i in range(tiles):
            cols = pl.ds(i * tile, tile)
            gate_sum[:, cols] = jnp.dot(
                x, w_gate[0:half_width, cols], preferred_element_type=jnp.float32
            )
            up_sum[:, cols] = jnp.dot(
                x, w_up[0:half_width, cols], preferred_element_type=jnp.float32
            )

    def multiply(k, between, begun=False):
        if not begun:
            landed(k, 0)
        landed(k, 1)
        start = half_width if begun else 0
        x = rows[peer[k], :, :, start:width].reshape(block_rows, width - start)
        for i in range(tiles):
            cols = pl.ds(i * tile, tile)
            gate = jnp.dot(x, w_gate[start:width, cols], preferred_element_type=jnp.float32)
            up = jnp.dot(x, w_up[start:width, cols], preferred_element_type=jnp.float32)
            if begun:
                gate = gate + gate_sum[:, cols]
                up = up + up_sum[:, cols]
            hidden[:, cols] = (gate / (1.0 + jnp.exp(-gate)) * up).astype(jnp.bfloat16)
        for act in between:
            act()
        if k == 0:
            weights[2].wait()
        for own_plane in (0, 1):
            there = plane if own_plane else 1 - plane
            for c in range(2):
                cols = pl.ds(
                    pl.multiple_of((2 * there + c) * slice_width, slice_width), slice_width
                )
                product = jnp.dot(hidden[...], w_down[:, cols], preferred_element_type=jnp.float32)
                part[k, there, c] = product.astype(jnp.bfloat16)
            pair_back(k, own_plane).start()

    def cross(k, half):
        other = 1 - plane
        if half == 0:
            pair_back(k, 0).wait_recv()
        for h in in_half(half):
            cross_out[k, lines(h)] = (
                part[k, other, core, lines(h)].astype(jnp.float32)
                + pair_in[k, other, lines(h)].astype(jnp.float32)
            ).astype(jnp.bfloat16)
            x_back(k, h).start()

    def give_back(k, half):
        if half == 0:
            pair_back(k, 1).wait_recv()
        for h in in_half(half):
            x_back(k, h).wait_recv()
            result = (
                part[k, plane, core, lines(h)].astype(jnp.float32)
                + pair_in[k, plane, lines(h)].astype(jnp.float32)
                + cross_in[k, lines(h)].astype(jnp.float32)
            ).astype(jnp.bfloat16)
            if k == 0:
                home[z, lines(h)] = result
            else:
                home_out[k, lines(h)] = result
                z_back(k, lines(h), True).start()

    def count_earlier():
        routes = table[:, 0:choose]
        lane = lax.broadcasted_iota(jnp.int32, (total, 128), 1).astype(jnp.float32)
        hit = ((routes[:, 0:1] == lane) | (routes[:, 1:2] == lane)).astype(jnp.float32)
        row_id = lax.broadcasted_iota(jnp.int32, (total, total), 0)
        col_id = lax.broadcasted_iota(jnp.int32, (total, total), 1)
        before = ((col_id < row_id) & (col_id // count == row_id // count)).astype(jnp.float32)
        earlier_ref[...] = jnp.dot(
            before.astype(jnp.bfloat16),
            hit.astype(jnp.bfloat16),
            preferred_element_type=jnp.float32,
        )

    def join(k):
        z_back(k, pl.ds(0, block_rows), False).wait_recv()

    def combine(k, first):
        if k:
            join(k)
        e = peer[k]
        expert = e.astype(jnp.float32)
        mine = table[:, 0:choose] == expert
        lanes = lax.broadcasted_iota(jnp.int32, (total, 128), 1).astype(jnp.float32)
        slot = jnp.sum(jnp.where(lanes == expert, earlier_ref[...], 0.0), axis=1, keepdims=True)
        block = lax.broadcasted_iota(jnp.int32, (total, 1), 0) // count
        named = jnp.max(mine.astype(jnp.float32), axis=1, keepdims=True)
        target = jnp.where(
            named > 0.0, slot + (block * capacity).astype(jnp.float32), jnp.float32(-1.0)
        )
        weight = jnp.sum(jnp.where(mine, table[:, choose : 2 * choose], 0.0), axis=1, keepdims=True)
        place = lax.broadcasted_iota(jnp.int32, (total, block_rows), 1).astype(jnp.float32)
        pick = (place == target).astype(jnp.float32).astype(jnp.bfloat16)
        term = weight * jnp.dot(pick, home[e], preferred_element_type=jnp.float32)
        combined[...] = term if first else combined[...] + term

    def todo(act, *arguments, where=None):
        def run():
            if where is None:
                act(*arguments)
            else:
                pl.when(is_end if where == "end" else jnp.logical_not(is_end))(
                    lambda: act(*arguments)
                )

        return run

    def end(act, *arguments):
        return todo(act, *arguments, where="end")

    def middle(act, *arguments):
        return todo(act, *arguments, where="middle")

    def send(k):
        for h in range(pieces):
            z_in(k, h, True).start()

    for h in range(2):
        spread(0, h)
    end(send, 2)()
    middle(send, 3)()
    middle(send, 1)()
    middle(send, 2)()
    for copy in weights:
        copy.start()
    count_earlier()
    spread(1, 0)
    relay(0, 0)
    spread(1, 1)
    relay(0, 1)
    weights[0].wait()
    weights[1].wait()
    multiply(0, [end(send, 1), end(send, 3), todo(spread, 2, 0)])
    relay(1, 0)
    relay(1, 1)
    spread(2, 1)
    end(cross, 0, 0)()
    multiply(1, [todo(relay, 2, 0), middle(spread, 3, 0)])
    relay(2, 1)
    middle(spread, 3, 1)()
    cross(1, 0)
    cross(1, 1)
    multiply(2, [middle(relay, 3, 0), end(spread, 3, 0)])
    end(spread, 3, 1)()
    end(give_back, 1, 0)()
    end(give_back, 1, 1)()
    middle(relay, 3, 1)()
    cross(2, 0)
    cross(2, 1)
    middle(give_back, 1, 0)()
    end(relay, 3, 0)()
    begin(3)
    end(relay, 3, 1)()
    multiply(3, [middle(give_back, 1, 1)], True)
    cross(3, 0)
    cross(3, 1)
    give_back(2, 0)
    give_back(2, 1)
    middle(cross, 0, 0)()
    cross(0, 1)
    give_back(3, 0)
    give_back(3, 1)
    combine(2, True)
    give_back(0, 0)
    give_back(0, 1)
    combine(0, False)
    combine(1, False)
    combine(3, False)

    small[4].wait()
    value = combined[...]
    folded = sum(
        value[:, i : i + 128] * value[:, i : i + 128] for i in range(0, slice_width, 128)
    )
    ones = jnp.ones((8, 128), jnp.float32)
    squares[q] = lax.dot_general(
        ones,
        folded,
        (((1,), (1,)), ((), ())),
        preferred_element_type=jnp.float32,
        precision=lax.Precision.HIGHEST,
    )

    def share(step, rows_of):
        return remote(
            squares.at[rows_of],
            squares.at[rows_of],
            sq_send.at[0],
            sq_recv.at[step],
            {"tp": lax.rem(q + step, groups)},
        )

    for step in range(1, groups):
        share(step, pl.ds(q, 1)).start()
    for step in range(1, groups):
        share(step, pl.ds(q, 1)).wait_recv()
    summed = squares[0]
    for i in range(1, groups):
        summed = summed + squares[i]
    scale = lax.rsqrt(summed / width + EPS)
    column = jnp.transpose(scale)[:, 0:1]
    out_ref[...] = (combined[...] * column * gain_out_ref[...]).astype(jnp.bfloat16)

    def drain(block, semaphore):
        remote(block, block, semaphore.at[0], semaphore.at[0], {"tp": across}).wait_send()

    drain(picked.at[0 : experts - 1], d1_send)
    drain(rows.at[0], d2x_send)
    drain(rows.at[0], d2p_send)
    drain(rows.at[0], d3_send)
    drain(pair_in, r1_send)
    drain(cross_out, r2_send)
    drain(home_out.at[1:experts], r3_send)
    drain(squares.at[1:groups], sq_send)


def fused(tokens, gain_in, routes, gates, w_gate, w_up, w_down, gain_out, capacity):
    experts = lax.axis_size("ep")
    groups = lax.axis_size("tp")
    count, width = tokens.shape
    total = routes.shape[0]
    hidden_width = w_gate.shape[2]
    slice_width = width // groups
    block_rows = groups * capacity
    bf16, f32 = jnp.bfloat16, jnp.float32
    vmem = pl.BlockSpec(memory_space=pltpu.VMEM)
    hbm = pl.BlockSpec(memory_space=pl.ANY)
    dma = pltpu.SemaphoreType.DMA
    return pl.pallas_call(
        functools.partial(fused_kernel, experts, groups, capacity),
        out_shape=jax.ShapeDtypeStruct((total, slice_width), bf16),
        in_specs=[hbm] * 8,
        out_specs=vmem,
        scratch_shapes=[
            pltpu.VMEM(tokens.shape, bf16),
            pltpu.VMEM((1, width), f32),
            pltpu.VMEM((routes.shape[1], total), jnp.int32),
            pltpu.VMEM((routes.shape[1], total), f32),
            pltpu.VMEM((1, slice_width), f32),
            pltpu.VMEM((8, total), f32),
            pltpu.VMEM((total, 8), f32),
            pltpu.VMEM((width, hidden_width), bf16),
            pltpu.VMEM((width, hidden_width), bf16),
            pltpu.VMEM((hidden_width, width), bf16),
            pltpu.VMEM((total, 128), f32),
            pltpu.VMEM((experts, capacity, width), bf16),
            pltpu.VMEM((experts, groups, capacity, width), bf16),
            pltpu.VMEM((block_rows, hidden_width), bf16),
            pltpu.VMEM((experts, groups // 2, 2, block_rows, slice_width), bf16),
            pltpu.VMEM((experts, groups // 2, block_rows, slice_width), bf16),
            pltpu.VMEM((experts, block_rows, slice_width), bf16),
            pltpu.VMEM((experts, block_rows, slice_width), bf16),
            pltpu.VMEM((experts, block_rows, slice_width), bf16),
            pltpu.VMEM((experts, block_rows, slice_width), bf16),
            pltpu.VMEM((total, slice_width), f32),
            pltpu.VMEM((block_rows, hidden_width), f32),
            pltpu.VMEM((block_rows, hidden_width), f32),
            pltpu.VMEM((groups, 8, total), f32),
            dma((3,)),
            dma((5,)),
            dma((1,)),
            dma((experts, 4)),
            dma((1,)),
            dma((experts, 2)),
            dma((1,)),
            dma((experts, 4)),
            dma((1,)),
            dma((experts, 2)),
            dma((1,)),
            dma((experts, 2)),
            dma((1,)),
            dma((experts, 4)),
            dma((1,)),
            dma((experts,)),
            dma((1,)),
            dma((groups,)),
        ],
        compiler_params=pltpu.CompilerParams(
            collective_id=0, has_side_effects=True, vmem_limit_bytes=48000 * 1024
        ),
    )(
        *(
            pltpu.with_memory_space_constraint(array, pltpu.HBM)
            for array in (
                tokens,
                gain_in[None],
                routes.T,
                gates.T,
                w_gate,
                w_up,
                w_down,
                gain_out[None],
            )
        )
    )


def local(tokens, gain_in, routes, gates, w_gate, w_up, w_down, gain_out):
    count, width = tokens.shape
    choose = routes.shape[1]
    experts = lax.axis_size("ep")
    groups = lax.axis_size("tp")
    capacity = (3 * count * choose + 2 * experts - 1) // (2 * experts)
    hidden_width = w_gate.shape[2]
    if experts == 4 and groups == 4 and choose == 2 and capacity % 16 == 0 and hidden_width % 256 == 0:
        return fused(
            tokens, gain_in, routes, gates, w_gate, w_up, w_down, gain_out, capacity
        )
    values = tokens.astype(jnp.float32)
    normed = (
        values * lax.rsqrt(jnp.mean(values * values, axis=-1, keepdims=True) + EPS) * gain_in
    ).astype(jnp.bfloat16)
    positions = slot_table(routes.reshape(groups, count, choose), experts, capacity)
    own = lax.dynamic_index_in_dim(positions, lax.axis_index("tp"), 0, keepdims=False)
    slots = jnp.arange(experts * capacity, dtype=jnp.int32)
    select = jnp.sum((own[None, :, :] == slots[:, None, None]).astype(jnp.bfloat16), axis=2)
    outgoing = jnp.dot(select, normed, preferred_element_type=jnp.float32).astype(jnp.bfloat16)
    outgoing = outgoing.reshape(experts, capacity, width)
    arrived = lax.all_to_all(outgoing, "ep", split_axis=0, concat_axis=0, tiled=True)
    piece = lax.all_gather(arrived[:, None], "tp", axis=1, tiled=True)
    flat = piece.reshape(-1, width)
    gate = jnp.dot(flat, w_gate[0], preferred_element_type=jnp.float32)
    up = jnp.dot(flat, w_up[0], preferred_element_type=jnp.float32)
    hidden = (jax.nn.silu(gate) * up).astype(jnp.bfloat16)
    hidden = hidden.reshape(piece.shape[:-1] + (hidden_width,))
    partial_value = jnp.dot(
        hidden.reshape(-1, hidden_width), w_down[0], preferred_element_type=jnp.float32
    )
    summed = lax.psum_scatter(
        partial_value.astype(jnp.bfloat16), "tp", scatter_dimension=1, tiled=True
    )
    slice_width = width // groups
    expert_out = summed.reshape(experts, groups * capacity, slice_width)
    returned = lax.all_to_all(expert_out, "ep", split_axis=0, concat_axis=0, tiled=True)
    returned = returned.reshape(experts, groups, capacity, slice_width).transpose(1, 0, 2, 3)
    returned = returned.reshape(groups, experts * capacity, slice_width).astype(jnp.float32)
    weights = gates.reshape(groups, count, choose)
    combine = jnp.sum(
        jnp.where(
            positions[..., None] == slots[None, None, None, :], weights[..., None], jnp.float32(0.0)
        ),
        axis=2,
    )
    combined = jnp.einsum("gtp,gpd->gtd", combine, returned, precision=lax.Precision.HIGHEST)
    combined = combined.reshape(groups * count, slice_width)
    squares = lax.psum(jnp.sum(combined * combined, axis=1), "tp")
    scale = lax.rsqrt(squares / width + EPS)
    return (combined * scale[:, None] * gain_out).astype(jnp.bfloat16)


def solution(mesh):
    in_specs = (
        P(("grp", "ep", "tp"), None),
        P(),
        P(("grp", "ep"), None),
        P(("grp", "ep"), None),
        P("ep", None, "tp"),
        P("ep", None, "tp"),
        P("ep", "tp", None),
        P("tp"),
    )
    out_specs = P(("grp", "ep"), "tp")
    return jax.shard_map(local, mesh=mesh, in_specs=in_specs, out_specs=out_specs, check_vma=False)
```

```python
import functools

import jax
import jax.numpy as jnp
from jax import lax
from jax.experimental import pallas as pl
from jax.experimental.pallas import tpu as pltpu
from jax.sharding import PartitionSpec as P

EPS = 1e-06


def slot_table(routes, experts, capacity):
    sources, count, choose = routes.shape
    flat = routes.reshape(sources, count * choose)
    onehot = (flat[:, :, None] == jnp.arange(experts, dtype=jnp.int32)[None, None, :]).astype(
        jnp.int32
    )
    earlier = jnp.cumsum(onehot, axis=1) - onehot
    slot = jnp.sum(earlier * onehot, axis=2)
    return (flat * capacity + slot).reshape(sources, count, choose)


MESH = pl.DeviceIdType.MESH


def fused_kernel(
    experts,
    groups,
    capacity,
    tokens_hbm,
    gain_in_hbm,
    routes_hbm,
    gates_hbm,
    w_gate_hbm,
    w_up_hbm,
    w_down_hbm,
    gain_out_hbm,
    out_ref,
    tokens_ref,
    gain_in_ref,
    routes_ref,
    gates_ref,
    gain_out_ref,
    stage,
    table,
    w_gate,
    w_up,
    w_down,
    earlier_ref,
    picked,
    rows,
    hidden,
    part,
    pair_in,
    cross_out,
    cross_in,
    home_out,
    home,
    combined,
    gate_sum,
    up_sum,
    squares,
    weight_sem,
    small_sem,
    d1_send,
    d1_recv,
    d2p_send,
    d2p_recv,
    d2x_send,
    d2x_recv,
    d3_send,
    d3_recv,
    r1_send,
    r1_recv,
    r2_send,
    r2_recv,
    r3_send,
    r3_recv,
    sq_send,
    sq_recv,
):
    z = lax.axis_index("ep")
    q = lax.axis_index("tp")
    core = lax.rem(q, 2)
    plane = q // 2
    partner = q + 1 - 2 * core
    across = lax.rem(q + 2, groups)
    count, width = tokens_ref.shape
    total = out_ref.shape[0]
    choose = routes_ref.shape[0]
    hidden_width = w_gate.shape[1]
    slice_width = out_ref.shape[1]
    block_rows = groups * capacity
    pieces = d1_recv.shape[1]
    per_half = pieces // 2
    piece_width = width // pieces
    piece_rows = block_rows // pieces

    last = experts - 1
    side = z // 2
    inward = z + side * (last - 2 * z)
    near = [inward, 2 - 2 * inward, 1 + inward, last + 0 * inward]
    peer = [p + side * (last - 2 * p) for p in near]
    is_end = inward == 0

    small = [
        pltpu.make_async_copy(src, dst, small_sem.at[i])
        for i, (src, dst) in enumerate(
            (
                (tokens_hbm, tokens_ref),
                (routes_hbm, routes_ref),
                (gates_hbm, gates_ref),
                (gain_in_hbm, gain_in_ref),
                (gain_out_hbm, gain_out_ref),
            )
        )
    ]
    for copy in small:
        copy.start()
    weights = [
        pltpu.make_async_copy(src.at[0], dst, weight_sem.at[i])
        for i, (src, dst) in enumerate(
            ((w_gate_hbm, w_gate), (w_up_hbm, w_up), (w_down_hbm, w_down))
        )
    ]
    barrier = pltpu.get_barrier_semaphore()
    for step in range(1, experts):
        pl.semaphore_signal(
            barrier, inc=1, device_id={"ep": lax.rem(z + step, experts)}, device_id_type=MESH
        )
    for step in range(1, groups):
        pl.semaphore_signal(
            barrier, inc=1, device_id={"tp": lax.rem(q + step, groups)}, device_id_type=MESH
        )

    for i in (1, 2, 0, 3):
        small[i].wait()
    stage[...] = jnp.zeros_like(stage)
    stage[0:choose, :] = routes_ref[...].astype(jnp.float32)
    stage[choose : 2 * choose, :] = gates_ref[...]
    table[...] = jnp.transpose(stage[...])
    own = pl.ds(pl.multiple_of(q * count, count), count)
    own_routes = table[own, :]
    own_lane = lax.broadcasted_iota(jnp.int32, (count, 128), 1).astype(jnp.float32)
    own_hit = (own_routes[:, 0:1] == own_lane) | (own_routes[:, 1:2] == own_lane)
    own_row = lax.broadcasted_iota(jnp.int32, (count, count), 0)
    own_col = lax.broadcasted_iota(jnp.int32, (count, count), 1)
    own_earlier = jnp.dot(
        (own_col < own_row).astype(jnp.float32).astype(jnp.bfloat16),
        own_hit.astype(jnp.float32).astype(jnp.bfloat16),
        preferred_element_type=jnp.float32,
    )
    slots = lax.broadcasted_iota(jnp.int32, (count, experts * capacity), 1).astype(jnp.float32)
    select = jnp.zeros((count, experts * capacity), jnp.float32)
    for k in range(choose):
        expert = own_routes[:, k : k + 1]
        slot = jnp.sum(
            jnp.where(own_lane == expert, own_earlier, 0.0), axis=1, keepdims=True
        )
        select = jnp.where(slots == expert * capacity + slot, 1.0, select)

    values = tokens_ref[...].astype(jnp.float32)
    normed = (
        values
        * lax.rsqrt(jnp.mean(values * values, axis=-1, keepdims=True) + EPS)
        * gain_in_ref[...]
    ).astype(jnp.bfloat16)
    picked[...] = (
        lax.dot_general(
            select.astype(jnp.bfloat16),
            normed,
            (((0,), (0,)), ((), ())),
            preferred_element_type=jnp.float32,
        )
        .astype(jnp.bfloat16)
        .reshape(experts, capacity, width)
    )
    rows[z, q] = picked[z]

    pl.semaphore_wait(barrier, experts - 1 + groups - 1)

    def remote(src, dst, send, recv, where):
        return pltpu.make_async_remote_copy(
            src_ref=src,
            dst_ref=dst,
            send_sem=send,
            recv_sem=recv,
            device_id=where,
            device_id_type=MESH,
        )

    def columns(h):
        return pl.ds(h * piece_width, piece_width)

    def lines(h):
        return pl.ds(h * piece_rows, piece_rows)

    def in_half(half):
        return range(half * per_half, (half + 1) * per_half)

    def z_in(k, h, outward):
        there = peer[k]
        where = z if outward else there
        return remote(
            picked.at[there, :, columns(h)],
            rows.at[where, q, :, columns(h)],
            d1_send.at[0],
            d1_recv.at[where, h],
            {"ep": there},
        )

    def x_in(k, h):
        block = rows.at[peer[k], q, :, columns(h)]
        return remote(block, block, d2x_send.at[0], d2x_recv.at[k, h], {"tp": across})

    def pair_of(k, cols, h):
        block = rows.at[peer[k], q, :, cols]
        return remote(block, block, d2p_send.at[0], d2p_recv.at[k, h // per_half], {"tp": partner})

    def pair_across(k, cols, h):
        block = rows.at[peer[k], across, :, cols]
        return remote(block, block, d3_send.at[0], d3_recv.at[k, h // per_half], {"tp": partner})

    def spread(k, half):
        for h in in_half(half):
            if k:
                z_in(k, h, False).wait_recv()
            x_in(k, h).start()
            pair_of(k, columns(h), h).start()

    def relay(k, half):
        for h in in_half(half):
            x_in(k, h).wait_recv()
            pair_across(k, columns(h), h).start()

    def pair_back(k, own_plane):
        there = plane if own_plane else 1 - plane
        return remote(
            part.at[k, there, 1 - core],
            pair_in.at[k, there],
            r1_send.at[0],
            r1_recv.at[k, own_plane],
            {"tp": partner},
        )

    def x_back(k, h):
        return remote(
            cross_out.at[k, lines(h)],
            cross_in.at[k, lines(h)],
            r2_send.at[0],
            r2_recv.at[k, h],
            {"tp": across},
        )

    def z_back(k, rows_of, outward):
        there = peer[k]
        where = z if outward else there
        return remote(
            home_out.at[k, rows_of],
            home.at[where, rows_of],
            r3_send.at[0],
            r3_recv.at[where],
            {"ep": there},
        )

    tile = 256
    tiles = hidden_width // tile

    half_width = width // 2

    def landed(k, half):
        cols = pl.ds(half * half_width, half_width)
        pair_of(k, cols, half * per_half).wait_recv()
        pair_across(k, cols, half * per_half).wait_recv()

    def begin(k):
        landed(k, 0)
        x = rows[peer[k], :, :, 0:half_width].reshape(block_rows, half_width)
        for i in range(tiles):
            cols = pl.ds(i * tile, tile)
            gate_sum[:, cols] = jnp.dot(
                x, w_gate[0:half_width, cols], preferred_element_type=jnp.float32
            )
            up_sum[:, cols] = jnp.dot(
                x, w_up[0:half_width, cols], preferred_element_type=jnp.float32
            )

    def multiply(k, between, begun=False):
        if not begun:
            landed(k, 0)
        landed(k, 1)
        start = half_width if begun else 0
        x = rows[peer[k], :, :, start:width].reshape(block_rows, width - start)
        for i in range(tiles):
            cols = pl.ds(i * tile, tile)
            gate = jnp.dot(x, w_gate[start:width, cols], preferred_element_type=jnp.float32)
            up = jnp.dot(x, w_up[start:width, cols], preferred_element_type=jnp.float32)
            if begun:
                gate = gate + gate_sum[:, cols]
                up = up + up_sum[:, cols]
            hidden[:, cols] = (gate / (1.0 + jnp.exp(-gate)) * up).astype(jnp.bfloat16)
        for act in between:
            act()
        if k == 0:
            weights[2].wait()
        for own_plane in (0, 1):
            there = plane if own_plane else 1 - plane
            for c in range(2):
                cols = pl.ds(
                    pl.multiple_of((2 * there + c) * slice_width, slice_width), slice_width
                )
                product = jnp.dot(hidden[...], w_down[:, cols], preferred_element_type=jnp.float32)
                part[k, there, c] = product.astype(jnp.bfloat16)
            pair_back(k, own_plane).start()

    def cross(k, half):
        other = 1 - plane
        if half == 0:
            pair_back(k, 0).wait_recv()
        for h in in_half(half):
            cross_out[k, lines(h)] = (
                part[k, other, core, lines(h)].astype(jnp.float32)
                + pair_in[k, other, lines(h)].astype(jnp.float32)
            ).astype(jnp.bfloat16)
            x_back(k, h).start()

    def give_back(k, half):
        if half == 0:
            pair_back(k, 1).wait_recv()
        for h in in_half(half):
            x_back(k, h).wait_recv()
            result = (
                part[k, plane, core, lines(h)].astype(jnp.float32)
                + pair_in[k, plane, lines(h)].astype(jnp.float32)
                + cross_in[k, lines(h)].astype(jnp.float32)
            ).astype(jnp.bfloat16)
            if k == 0:
                home[z, lines(h)] = result
            else:
                home_out[k, lines(h)] = result
                z_back(k, lines(h), True).start()

    def count_earlier():
        routes = table[:, 0:choose]
        lane = lax.broadcasted_iota(jnp.int32, (total, 128), 1).astype(jnp.float32)
        hit = ((routes[:, 0:1] == lane) | (routes[:, 1:2] == lane)).astype(jnp.float32)
        row_id = lax.broadcasted_iota(jnp.int32, (total, total), 0)
        col_id = lax.broadcasted_iota(jnp.int32, (total, total), 1)
        before = ((col_id < row_id) & (col_id // count == row_id // count)).astype(jnp.float32)
        earlier_ref[...] = jnp.dot(
            before.astype(jnp.bfloat16),
            hit.astype(jnp.bfloat16),
            preferred_element_type=jnp.float32,
        )

    def join(k):
        z_back(k, pl.ds(0, block_rows), False).wait_recv()

    def combine(k, first):
        e = peer[k]
        expert = e.astype(jnp.float32)
        mine = table[:, 0:choose] == expert
        lanes = lax.broadcasted_iota(jnp.int32, (total, 128), 1).astype(jnp.float32)
        slot = jnp.sum(jnp.where(lanes == expert, earlier_ref[...], 0.0), axis=1, keepdims=True)
        block = lax.broadcasted_iota(jnp.int32, (total, 1), 0) // count
        named = jnp.max(mine.astype(jnp.float32), axis=1, keepdims=True)
        target = jnp.where(
            named > 0.0, slot + (block * capacity).astype(jnp.float32), jnp.float32(-1.0)
        )
        weight = jnp.sum(jnp.where(mine, table[:, choose : 2 * choose], 0.0), axis=1, keepdims=True)
        place = lax.broadcasted_iota(jnp.int32, (total, block_rows), 1).astype(jnp.float32)
        pick = (place == target).astype(jnp.float32).astype(jnp.bfloat16)
        if k:
            join(k)
        term = weight * jnp.dot(pick, home[e], preferred_element_type=jnp.float32)
        combined[...] = term if first else combined[...] + term

    def todo(act, *arguments, where=None):
        def run():
            if where is None:
                act(*arguments)
            else:
                pl.when(is_end if where == "end" else jnp.logical_not(is_end))(
                    lambda: act(*arguments)
                )

        return run

    def end(act, *arguments):
        return todo(act, *arguments, where="end")

    def middle(act, *arguments):
        return todo(act, *arguments, where="middle")

    def send(k):
        for h in range(pieces):
            z_in(k, h, True).start()

    for h in range(2):
        spread(0, h)
    end(send, 2)()
    middle(send, 3)()
    middle(send, 1)()
    middle(send, 2)()
    for copy in weights:
        copy.start()
    count_earlier()
    spread(1, 0)
    relay(0, 0)
    spread(1, 1)
    relay(0, 1)
    weights[0].wait()
    weights[1].wait()
    multiply(0, [end(send, 1), end(send, 3), todo(spread, 2, 0)])
    relay(1, 0)
    relay(1, 1)
    spread(2, 1)
    end(cross, 0, 0)()
    multiply(1, [todo(relay, 2, 0), middle(spread, 3, 0)])
    relay(2, 1)
    middle(spread, 3, 1)()
    cross(1, 0)
    cross(1, 1)
    multiply(2, [middle(relay, 3, 0)])
    end(spread, 3, 0)()
    end(give_back, 1, 0)()
    end(spread, 3, 1)()
    end(give_back, 1, 1)()
    middle(relay, 3, 1)()
    cross(2, 0)
    cross(2, 1)
    middle(give_back, 1, 0)()
    end(relay, 3, 0)()
    begin(3)
    end(relay, 3, 1)()
    multiply(3, [end(give_back, 2, 0), middle(give_back, 1, 1)], True)
    cross(3, 0)
    cross(3, 1)
    middle(give_back, 2, 0)()
    give_back(2, 1)
    middle(cross, 0, 0)()
    cross(0, 1)
    give_back(3, 0)
    give_back(3, 1)
    combine(2, True)
    give_back(0, 0)
    give_back(0, 1)
    combine(0, False)
    combine(1, False)
    combine(3, False)

    small[4].wait()
    value = combined[...]
    folded = sum(
        value[:, i : i + 128] * value[:, i : i + 128] for i in range(0, slice_width, 128)
    )
    ones = jnp.ones((8, 128), jnp.float32)
    squares[q] = lax.dot_general(
        ones,
        folded,
        (((1,), (1,)), ((), ())),
        preferred_element_type=jnp.float32,
        precision=lax.Precision.HIGHEST,
    )

    def share(step, rows_of):
        return remote(
            squares.at[rows_of],
            squares.at[rows_of],
            sq_send.at[0],
            sq_recv.at[step],
            {"tp": lax.rem(q + step, groups)},
        )

    for step in range(1, groups):
        share(step, pl.ds(q, 1)).start()
    for step in range(1, groups):
        share(step, pl.ds(q, 1)).wait_recv()
    summed = squares[0]
    for i in range(1, groups):
        summed = summed + squares[i]
    scale = lax.rsqrt(summed / width + EPS)
    column = jnp.transpose(scale)[:, 0:1]
    out_ref[...] = (combined[...] * column * gain_out_ref[...]).astype(jnp.bfloat16)

    def drain(block, semaphore):
        remote(block, block, semaphore.at[0], semaphore.at[0], {"tp": across}).wait_send()

    drain(picked.at[0 : experts - 1], d1_send)
    drain(rows.at[0], d2x_send)
    drain(rows.at[0], d2p_send)
    drain(rows.at[0], d3_send)
    drain(pair_in, r1_send)
    drain(cross_out, r2_send)
    drain(home_out.at[1:experts], r3_send)
    drain(squares.at[1:groups], sq_send)


def fused(tokens, gain_in, routes, gates, w_gate, w_up, w_down, gain_out, capacity):
    experts = lax.axis_size("ep")
    groups = lax.axis_size("tp")
    count, width = tokens.shape
    total = routes.shape[0]
    hidden_width = w_gate.shape[2]
    slice_width = width // groups
    block_rows = groups * capacity
    bf16, f32 = jnp.bfloat16, jnp.float32
    vmem = pl.BlockSpec(memory_space=pltpu.VMEM)
    hbm = pl.BlockSpec(memory_space=pl.ANY)
    dma = pltpu.SemaphoreType.DMA
    return pl.pallas_call(
        functools.partial(fused_kernel, experts, groups, capacity),
        out_shape=jax.ShapeDtypeStruct((total, slice_width), bf16),
        in_specs=[hbm] * 8,
        out_specs=vmem,
        scratch_shapes=[
            pltpu.VMEM(tokens.shape, bf16),
            pltpu.VMEM((1, width), f32),
            pltpu.VMEM((routes.shape[1], total), jnp.int32),
            pltpu.VMEM((routes.shape[1], total), f32),
            pltpu.VMEM((1, slice_width), f32),
            pltpu.VMEM((8, total), f32),
            pltpu.VMEM((total, 8), f32),
            pltpu.VMEM((width, hidden_width), bf16),
            pltpu.VMEM((width, hidden_width), bf16),
            pltpu.VMEM((hidden_width, width), bf16),
            pltpu.VMEM((total, 128), f32),
            pltpu.VMEM((experts, capacity, width), bf16),
            pltpu.VMEM((experts, groups, capacity, width), bf16),
            pltpu.VMEM((block_rows, hidden_width), bf16),
            pltpu.VMEM((experts, groups // 2, 2, block_rows, slice_width), bf16),
            pltpu.VMEM((experts, groups // 2, block_rows, slice_width), bf16),
            pltpu.VMEM((experts, block_rows, slice_width), bf16),
            pltpu.VMEM((experts, block_rows, slice_width), bf16),
            pltpu.VMEM((experts, block_rows, slice_width), bf16),
            pltpu.VMEM((experts, block_rows, slice_width), bf16),
            pltpu.VMEM((total, slice_width), f32),
            pltpu.VMEM((block_rows, hidden_width), f32),
            pltpu.VMEM((block_rows, hidden_width), f32),
            pltpu.VMEM((groups, 8, total), f32),
            dma((3,)),
            dma((5,)),
            dma((1,)),
            dma((experts, 4)),
            dma((1,)),
            dma((experts, 2)),
            dma((1,)),
            dma((experts, 4)),
            dma((1,)),
            dma((experts, 2)),
            dma((1,)),
            dma((experts, 2)),
            dma((1,)),
            dma((experts, 4)),
            dma((1,)),
            dma((experts,)),
            dma((1,)),
            dma((groups,)),
        ],
        compiler_params=pltpu.CompilerParams(
            collective_id=0, has_side_effects=True, vmem_limit_bytes=48000 * 1024
        ),
    )(
        *(
            pltpu.with_memory_space_constraint(array, pltpu.HBM)
            for array in (
                tokens,
                gain_in[None],
                routes.T,
                gates.T,
                w_gate,
                w_up,
                w_down,
                gain_out[None],
            )
        )
    )


def local(tokens, gain_in, routes, gates, w_gate, w_up, w_down, gain_out):
    count, width = tokens.shape
    choose = routes.shape[1]
    experts = lax.axis_size("ep")
    groups = lax.axis_size("tp")
    capacity = (3 * count * choose + 2 * experts - 1) // (2 * experts)
    hidden_width = w_gate.shape[2]
    if experts == 4 and groups == 4 and choose == 2 and capacity % 16 == 0 and hidden_width % 256 == 0:
        return fused(
            tokens, gain_in, routes, gates, w_gate, w_up, w_down, gain_out, capacity
        )
    values = tokens.astype(jnp.float32)
    normed = (
        values * lax.rsqrt(jnp.mean(values * values, axis=-1, keepdims=True) + EPS) * gain_in
    ).astype(jnp.bfloat16)
    positions = slot_table(routes.reshape(groups, count, choose), experts, capacity)
    own = lax.dynamic_index_in_dim(positions, lax.axis_index("tp"), 0, keepdims=False)
    slots = jnp.arange(experts * capacity, dtype=jnp.int32)
    select = jnp.sum((own[None, :, :] == slots[:, None, None]).astype(jnp.bfloat16), axis=2)
    outgoing = jnp.dot(select, normed, preferred_element_type=jnp.float32).astype(jnp.bfloat16)
    outgoing = outgoing.reshape(experts, capacity, width)
    arrived = lax.all_to_all(outgoing, "ep", split_axis=0, concat_axis=0, tiled=True)
    piece = lax.all_gather(arrived[:, None], "tp", axis=1, tiled=True)
    flat = piece.reshape(-1, width)
    gate = jnp.dot(flat, w_gate[0], preferred_element_type=jnp.float32)
    up = jnp.dot(flat, w_up[0], preferred_element_type=jnp.float32)
    hidden = (jax.nn.silu(gate) * up).astype(jnp.bfloat16)
    hidden = hidden.reshape(piece.shape[:-1] + (hidden_width,))
    partial_value = jnp.dot(
        hidden.reshape(-1, hidden_width), w_down[0], preferred_element_type=jnp.float32
    )
    summed = lax.psum_scatter(
        partial_value.astype(jnp.bfloat16), "tp", scatter_dimension=1, tiled=True
    )
    slice_width = width // groups
    expert_out = summed.reshape(experts, groups * capacity, slice_width)
    returned = lax.all_to_all(expert_out, "ep", split_axis=0, concat_axis=0, tiled=True)
    returned = returned.reshape(experts, groups, capacity, slice_width).transpose(1, 0, 2, 3)
    returned = returned.reshape(groups, experts * capacity, slice_width).astype(jnp.float32)
    weights = gates.reshape(groups, count, choose)
    combine = jnp.sum(
        jnp.where(
            positions[..., None] == slots[None, None, None, :], weights[..., None], jnp.float32(0.0)
        ),
        axis=2,
    )
    combined = jnp.einsum("gtp,gpd->gtd", combine, returned, precision=lax.Precision.HIGHEST)
    combined = combined.reshape(groups * count, slice_width)
    squares = lax.psum(jnp.sum(combined * combined, axis=1), "tp")
    scale = lax.rsqrt(squares / width + EPS)
    return (combined * scale[:, None] * gain_out).astype(jnp.bfloat16)


def solution(mesh):
    in_specs = (
        P(("grp", "ep", "tp"), None),
        P(),
        P(("grp", "ep"), None),
        P(("grp", "ep"), None),
        P("ep", None, "tp"),
        P("ep", None, "tp"),
        P("ep", "tp", None),
        P("tp"),
    )
    out_specs = P(("grp", "ep"), "tp")
    return jax.shard_map(local, mesh=mesh, in_specs=in_specs, out_specs=out_specs, check_vma=False)
```
